32 devices in a mesh: ep: 8 (over z, x), tp: 4 (over y, core).
Axes of the slice: x: 2, y: 2, z: 4, core: 2. Of those that a mesh axis runs over, the one named last changes fastest.
Arguments:
- tokens: bfloat16 [4096, 2048], P(('ep', 'tp')), may hold values from -6 to 6
- routes: int32 [4096, 2], P(('ep', 'tp')), may hold values from 0 to 31, as said below
- gates: float32 [4096, 2], P(('ep', 'tp')), may hold values from 0.1 to 0.6
- w_gate: bfloat16 [32, 2048, 768], P(('ep', 'tp')), may hold values from -0.125 to 0.125
- w_up: bfloat16 [32, 2048, 768], P(('ep', 'tp')), may hold values from -0.125 to 0.125
- w_down: bfloat16 [32, 768, 2048], P(('ep', 'tp')), may hold values from -0.21875 to 0.21875
- moe_out: bfloat16 [4096, 2048], P('ep', 'tp'), may hold values from -16 to 16
- norm_gain: float32 [2048], P('tp'), may hold values from 0.1 to 1.9
- out_grad: bfloat16 [4096, 2048], P('ep', 'tp'), may hold values from -16 to 16
Outputs:
- token_grad: bfloat16 [4096, 2048], P(('ep', 'tp'))
- gates_grad: bfloat16 [4096, 2], P(('ep', 'tp'))
- w_gate_grad: bfloat16 [32, 2048, 768], P(('ep', 'tp'))
- w_up_grad: bfloat16 [32, 2048, 768], P(('ep', 'tp'))
- w_down_grad: bfloat16 [32, 768, 2048], P(('ep', 'tp'))
The draws below stay inside these ranges and needn't reach their ends.
Inputs may be any that keep to these rules, and one draw needn't show every extreme that they name: `routes`: the two experts of a row differ and lie in one group (expert e is in group e // 8). In the 128 rows of one device the tokens fall into the groups in shares 3/8, 3/8, 1/8, 1/8 of 128, which group takes which share varying. In the rows of one device no expert is named more than 16 times, and one expert is named exactly 16 times in the rows of every device.
All inputs are finite; a program needn't handle non-finite values.
Results may differ from the reference program's by a relative error of at most 0.0071.
Values may be sent and summed in bfloat16 or wider, within the bound.
A program may use at most 128 MiB of HBM per device.

```python
import jax
import jax.numpy as jnp
from jax import lax

D = 2048
F = 768
GROUPS = 4
TOPK = 2
TOK_DEV = 128
EXPERTS = 32
EXP_GROUP = 8
CAP = 16
TOKENS = 4096


def draw_routes(key, part):
    tickets = EXP_GROUP * CAP
    shares = [3 * TOK_DEV // 8, 3 * TOK_DEV // 8, TOK_DEV // 8, TOK_DEV // 8]
    hot_global = jax.random.randint(jax.random.fold_in(key, 11), (), 0, EXPERTS)

    def one_block(block_key):
        sub_keys = jax.random.split(block_key, 4)
        group_order = jax.random.permutation(sub_keys[0], GROUPS)
        token_order = jax.random.permutation(sub_keys[1], TOK_DEV)
        hot_inner = jax.random.randint(sub_keys[2], (GROUPS,), 0, EXP_GROUP)
        noise_draw = jax.random.randint(sub_keys[3], (GROUPS, tickets), 0, 2 ** 19)
        ticket_ids = jnp.arange(tickets, dtype=jnp.int32)
        inner_ids = ticket_ids // CAP
        result = jnp.zeros((TOK_DEV, 2), jnp.int32)
        offset = 0
        for rank in range(GROUPS):
            expert_ids = group_order[rank] * EXP_GROUP + inner_ids
            hot_flag = jnp.logical_or(inner_ids == hot_inner[rank], expert_ids == hot_global).astype(jnp.int32)
            score_value = (hot_flag * 2 ** 19 + noise_draw[rank]) * tickets + ticket_ids
            share_size = shares[rank]
            picked = lax.top_k(score_value, 2 * share_size)[1]
            chosen = jnp.sort(expert_ids[picked])
            places = token_order[offset:offset + share_size]
            result = result.at[places, 0].set(chosen[:share_size])
            result = result.at[places, 1].set(chosen[share_size:])
            offset = offset + share_size
        return result
    block_keys = jax.random.split(jax.random.fold_in(key, 12), TOKENS // TOK_DEV)
    return jax.vmap(one_block)(block_keys).reshape(TOKENS, 2).astype(jnp.int32)


def paired_fields(key):
    sub_keys = jax.random.split(jax.random.fold_in(key, 21), 5)
    base = jax.random.normal(sub_keys[0], (TOKENS, D), jnp.float32)
    block_scale = jnp.exp(jax.random.uniform(sub_keys[1], (8,), jnp.float32, -1.2, 1.2))
    fine_scale = jnp.exp(jax.random.uniform(sub_keys[2], (D,), jnp.float32, -0.35, 0.35))
    columns = jnp.arange(D) * 8 // D
    col_scale = block_scale[columns] * fine_scale
    saved_out = jnp.clip(base * col_scale[None, :], -16.0, 16.0)
    noise_part = jax.random.normal(sub_keys[4], (TOKENS, D), jnp.float32)
    cotangent = jnp.clip(0.6 * base + 0.8 * noise_part, -16.0, 16.0)
    return (saved_out, cotangent)


def draw_moe_out(key, part):
    return paired_fields(key)[0].astype(jnp.bfloat16)


def draw_out_grad(key, part):
    return paired_fields(key)[1].astype(jnp.bfloat16)


def steps_of(key, shape, pieces, smallest, high):
    def one(dim, parts):
        draws = jax.random.uniform(jax.random.fold_in(jax.random.fold_in(key, 6), dim), (parts,), jnp.float32, smallest / len(pieces), high / len(pieces))
        return jnp.repeat(jnp.exp(draws), shape[dim] // parts).reshape((-1,) + (1,) * (len(shape) - dim - 1))

    loudness = one(*pieces[0])
    for cut in pieces[1:]:
        loudness = loudness * one(*cut)
    return loudness


def gaussian(key, extent, deviation, limit, shards=(), held_as=jnp.bfloat16):
    values = deviation * jax.random.normal(key, extent, jnp.float32)
    if shards:
        values = values * steps_of(key, extent, shards, -0.22, 0.18)
    return jnp.clip(values, -limit, limit).astype(held_as)


def setup_inputs(seed: int = 0) -> dict:
    arg_keys = jax.random.split(jax.random.key(seed), 10)
    tokens = gaussian(arg_keys[0], (TOKENS, D), 1.0, 6.0, ((0, 32),))
    routes = draw_routes(jax.random.fold_in(arg_keys[9], 71), 0)
    gates = jnp.clip(0.1 + 0.5 * jax.random.uniform(arg_keys[2], (TOKENS, TOPK), jnp.float32) ** steps_of(arg_keys[2], (TOKENS, TOPK), ((0, 32),), -0.2, 0.2), 0.1, 0.6)
    w_gate = gaussian(arg_keys[3], (EXPERTS, D, F), D ** -0.5, 0.125, ((0, 32),))
    w_up = gaussian(arg_keys[4], (EXPERTS, D, F), D ** -0.5, 0.125, ((0, 32),))
    w_down = gaussian(arg_keys[5], (EXPERTS, F, D), F ** -0.5, 0.21875, ((0, 32),))
    moe_out = draw_moe_out(jax.random.fold_in(arg_keys[9], 71), 0)
    norm_gain = jnp.clip(1.0 + 0.18 * jax.random.normal(arg_keys[7], (D,), jnp.float32), 0.1, 1.9)
    out_grad = draw_out_grad(jax.random.fold_in(arg_keys[9], 71), 0)
    return {"tokens": tokens, "routes": routes, "gates": gates, "w_gate": w_gate, "w_up": w_up, "w_down": w_down, "moe_out": moe_out, "norm_gain": norm_gain, "out_grad": out_grad}


epsilon = 1e-06
block_rows = 256

def contract(left, right, left_dim, right_dim):
    return lax.dot_general(left, right, (((left_dim,), (right_dim,)), ((), ())), preferred_element_type=jnp.float32)

def norm_backward(moe_out, norm_gain, out_grad):
    features = moe_out.shape[1]
    saved_out = moe_out.astype(jnp.float32)
    scaled = norm_gain.astype(jnp.float32)[None, :] * out_grad.astype(jnp.float32)
    square_sum = lax.optimization_barrier(jnp.sum(saved_out * saved_out, axis=1))
    cross_sum = lax.optimization_barrier(jnp.sum(saved_out * scaled, axis=1))
    inv_rms = lax.rsqrt(square_sum / features + epsilon)
    result = inv_rms[:, None] * scaled - saved_out * (inv_rms ** 3 * cross_sum / features)[:, None]
    return result.astype(jnp.bfloat16)

def expert_terms(row_block, cot_block, gate_row, w_gate_one, w_up_one, w_down_one):
    pre_gate = jnp.dot(row_block, w_gate_one, preferred_element_type=jnp.float32)
    pre_up = jnp.dot(row_block, w_up_one, preferred_element_type=jnp.float32)
    sigmoid_gate = jax.nn.sigmoid(pre_gate)
    activated = pre_gate * sigmoid_gate
    hidden = activated * pre_up
    hid_grad = contract(cot_block, w_down_one, 1, 1)
    gate_grad = lax.optimization_barrier(jnp.sum(hidden * hid_grad, axis=1)).astype(jnp.bfloat16)
    weight = gate_row.astype(jnp.float32)[:, None]
    d_hidden = weight * hid_grad
    d_gate = (d_hidden * pre_up * sigmoid_gate * (1.0 + pre_gate * (1.0 - sigmoid_gate))).astype(jnp.bfloat16)
    d_up = (d_hidden * activated).astype(jnp.bfloat16)
    token_back = (contract(d_gate, w_gate_one, 1, 1) + contract(d_up, w_up_one, 1, 1)).astype(jnp.bfloat16)
    scaled_cot = (weight * cot_block.astype(jnp.float32)).astype(jnp.bfloat16)
    grad_gate = contract(row_block, d_gate, 0, 0)
    grad_up = contract(row_block, d_up, 0, 0)
    grad_down = contract(hidden.astype(jnp.bfloat16), scaled_cot, 0, 0)
    return (token_back, gate_grad, grad_gate, grad_up, grad_down)

def reference(tokens, routes, gates, w_gate, w_up, w_down, moe_out, norm_gain, out_grad):
    features = tokens.shape[1]
    hidden_width = w_gate.shape[2]
    expert_cot = norm_backward(moe_out, norm_gain, out_grad)
    flat_ids = routes.reshape(-1).astype(jnp.int32)
    route_count = flat_ids.shape[0]
    flat_token = (jnp.arange(route_count, dtype=jnp.int32) // TOPK).astype(jnp.int32)
    flat_gate = gates.reshape(-1).astype(jnp.bfloat16)
    sorted_order = jnp.argsort(flat_ids, stable=True).astype(jnp.int32)
    totals = jnp.zeros((EXPERTS,), jnp.int32).at[flat_ids].add(1)
    starts = (jnp.cumsum(totals) - totals).astype(jnp.int32)
    token_pad = jnp.concatenate([tokens, jnp.zeros((1, features), jnp.bfloat16)], axis=0)
    cot_pad = jnp.concatenate([expert_cot, jnp.zeros((1, features), jnp.bfloat16)], axis=0)

    def per_expert(state_pair, inputs):
        expert_index, w_gate_one, w_up_one, w_down_one = inputs
        first_slot = starts[expert_index]
        load_size = totals[expert_index]

        def one_block(block_index, state):
            route_dx, route_gg, acc_gate, acc_up, acc_down = state
            position = (first_slot + block_index * block_rows + jnp.arange(block_rows, dtype=jnp.int32)).astype(jnp.int32)
            in_range = position < first_slot + load_size
            route_ids = sorted_order[jnp.clip(position, 0, route_count - 1)]
            token_ids = jnp.where(in_range, flat_token[route_ids], TOKENS).astype(jnp.int32)
            gate_row = jnp.where(in_range, flat_gate[route_ids], jnp.zeros((), jnp.bfloat16))
            target = jnp.where(in_range, route_ids, route_count).astype(jnp.int32)
            token_back, gate_grad, grad_gate, grad_up, grad_down = expert_terms(token_pad[token_ids], cot_pad[token_ids], gate_row, w_gate_one, w_up_one, w_down_one)
            route_dx = route_dx.at[target].set(token_back)
            route_gg = route_gg.at[target].set(gate_grad)
            return (route_dx, route_gg, acc_gate + grad_gate, acc_up + grad_up, acc_down + grad_down)
        blocks = (load_size + block_rows - 1) // block_rows
        start_state = (state_pair[0], state_pair[1], jnp.zeros((features, hidden_width), jnp.float32), jnp.zeros((features, hidden_width), jnp.float32), jnp.zeros((hidden_width, features), jnp.float32))
        route_dx, route_gg, acc_gate, acc_up, acc_down = lax.fori_loop(0, blocks, one_block, start_state)
        return ((route_dx, route_gg), (acc_gate.astype(jnp.bfloat16), acc_up.astype(jnp.bfloat16), acc_down.astype(jnp.bfloat16)))
    start_pair = (jnp.zeros((route_count + 1, features), jnp.bfloat16), jnp.zeros((route_count + 1,), jnp.bfloat16))
    final_pair, stacked = lax.scan(per_expert, start_pair, (jnp.arange(EXPERTS, dtype=jnp.int32), w_gate, w_up, w_down))
    route_dx, route_gg = final_pair
    token_grad = lax.optimization_barrier(jnp.sum(route_dx[:route_count].astype(jnp.float32).reshape(TOKENS, TOPK, features), axis=1)).astype(jnp.bfloat16)
    gates_grad = route_gg[:route_count].reshape(TOKENS, TOPK)
    return (token_grad, gates_grad, stacked[0], stacked[1], stacked[2])
```

```python
import functools

import jax
import jax.numpy as jnp
from jax import lax
from jax.experimental import pallas as pl
from jax.experimental.pallas import tpu as pltpu
from jax.sharding import Mesh
from jax.sharding import PartitionSpec as P

epsilon = 1e-06
groups = 4
MESH = pl.DeviceIdType.MESH
AXES = ("z", "x", "tp")


def contract(left, right, left_dim, right_dim):
    return lax.dot_general(
        left, right, (((left_dim,), (right_dim,)), ((), ())), preferred_element_type=jnp.float32
    )


def earlier_equal(ids):
    count = ids.shape[-1]
    place = jnp.arange(count, dtype=jnp.int32)
    same = (ids[..., :, None] == ids[..., None, :]) & (place[:, None] > place[None, :])
    return jnp.sum(same.astype(jnp.int32), axis=-1)


def places(plane_size):
    z, x, t = (lax.axis_index(name) for name in AXES)
    z_count, t_count = lax.axis_size("z"), lax.axis_size("tp")
    own = x * t_count + t

    def z_peer(d):
        return (lax.rem(z + d, z_count), x, t)

    def plane_peer(k):
        q = lax.rem(own + k, plane_size)
        return q, (z, q // t_count, lax.rem(q, t_count))

    return z, own, z_count, z_peer, plane_peer


def enter(z_count, plane_size, z_peer, plane_peer):
    barrier = pltpu.get_barrier_semaphore()
    for d in range(1, z_count):
        pl.semaphore_signal(barrier, inc=1, device_id=z_peer(d), device_id_type=MESH)

    def greet(k, carry):
        pl.semaphore_signal(barrier, inc=1, device_id=plane_peer(k)[1], device_id_type=MESH)
        return carry

    lax.fori_loop(1, plane_size, greet, 0)
    pl.semaphore_wait(barrier, z_count - 1 + plane_size - 1)


def columns_dot(left, read, write, features):
    chunk = min(512, features)

    def one(c, carry):
        cols = pl.ds(pl.multiple_of(c * chunk, chunk), chunk)
        write(cols, jnp.dot(left, read(cols), preferred_element_type=jnp.float32))
        return carry

    lax.fori_loop(0, features // chunk, one, 0)


def dispatch_kernel(
    plane_size, slots, tok_ref, cot_ref, sel_ref, tok_out, cot_out,
    zbuf, sbuf, zs_sem, zr_sem, ps_sem, pr_sem, loc_sem,
):
    z, own, z_count, z_peer, plane_peer = places(plane_size)
    features = tok_ref.shape[-1]
    sends, outs = (tok_ref, cot_ref), (tok_out, cot_out)
    enter(z_count, plane_size, z_peer, plane_peer)

    def z_copy(a, d):
        return pltpu.make_async_remote_copy(
            src_ref=sends[a].at[lax.rem(z + d, z_count)],
            dst_ref=zbuf.at[a, d],
            send_sem=zs_sem.at[a, d],
            recv_sem=zr_sem.at[a, d],
            device_id=z_peer(d),
            device_id_type=MESH,
        )

    def rows_of(q):
        return pl.ds(pl.multiple_of(q * slots, slots), slots)

    def plane_copy(a, d, k):
        q, device = plane_peer(k)
        src = lax.rem(z + z_count - d, z_count)
        return pltpu.make_async_remote_copy(
            src_ref=sbuf.at[a, d, rows_of(q)],
            dst_ref=outs[a].at[src, rows_of(own)],
            send_sem=ps_sem.at[a, d, k],
            recv_sem=pr_sem.at[a, d, k],
            device_id=device,
            device_id_type=MESH,
        )

    def own_copy(a, d):
        src = lax.rem(z + z_count - d, z_count)
        return pltpu.make_async_copy(
            sbuf.at[a, d, rows_of(own)], outs[a].at[src, rows_of(own)], loc_sem.at[a, d]
        )

    for a in range(2):
        for d in range(1, z_count):
            z_copy(a, d).start()
    for a, d in [(0, 0), (1, 0)] + [(a, d) for a in range(2) for d in range(1, z_count)]:
        src = lax.rem(z + z_count - d, z_count)
        if d:
            z_copy(a, d).wait_recv()

        def read(cols):
            return zbuf[a, d, :, cols] if d else sends[a][z, :, cols]

        def write(cols, value):
            sbuf[a, d, :, cols] = value.astype(sbuf.dtype)

        columns_dot(sel_ref[src], read, write, features)
        lax.fori_loop(1, plane_size, lambda k, c: (plane_copy(a, d, k).start(), c)[1], 0)
        own_copy(a, d).start()
    for a in range(2):
        for d in range(z_count):
            if d:
                z_copy(a, d).wait_send()
            own_copy(a, d).wait()
            lax.fori_loop(1, plane_size, lambda k, c: (plane_copy(a, d, k).wait(), c)[1], 0)


def combine_kernel(
    plane_size, slots, back_ref, comb_ref, out_ref,
    rbuf, cbuf, zs_sem, zr_sem, ps_sem, pr_sem, loc_sem, own_sem,
):
    z, own, z_count, z_peer, plane_peer = places(plane_size)
    features = back_ref.shape[-1]
    enter(z_count, plane_size, z_peer, plane_peer)

    def rows_of(q):
        return pl.ds(pl.multiple_of(q * slots, slots), slots)

    def plane_copy(d, k):
        q, device = plane_peer(k)
        return pltpu.make_async_remote_copy(
            src_ref=back_ref.at[lax.rem(z + d, z_count), rows_of(q)],
            dst_ref=rbuf.at[d, rows_of(own)],
            send_sem=ps_sem.at[d, k],
            recv_sem=pr_sem.at[d, k],
            device_id=device,
            device_id_type=MESH,
        )

    def own_rows(d):
        return pltpu.make_async_copy(
            back_ref.at[lax.rem(z + d, z_count), rows_of(own)], rbuf.at[d, rows_of(own)], loc_sem.at[d]
        )

    def z_copy(d):
        return pltpu.make_async_remote_copy(
            src_ref=cbuf.at[d],
            dst_ref=out_ref.at[z],
            send_sem=zs_sem.at[d],
            recv_sem=zr_sem.at[d],
            device_id=z_peer(d),
            device_id_type=MESH,
        )

    keep = pltpu.make_async_copy(cbuf.at[0], out_ref.at[z], own_sem)
    order = list(range(1, z_count)) + [0]
    for d in order:
        own_rows(d).start()
        lax.fori_loop(1, plane_size, lambda k, c: (plane_copy(d, k).start(), c)[1], 0)
    for d in order:
        own_rows(d).wait()
        lax.fori_loop(1, plane_size, lambda k, c: (plane_copy(d, k).wait_recv(), c)[1], 0)

        def read(cols):
            return rbuf[d, :, cols]

        def write(cols, value):
            cbuf[d, :, cols] = value.astype(cbuf.dtype)

        columns_dot(comb_ref[lax.rem(z + d, z_count)], read, write, features)
        if d:
            z_copy(d).start()
        else:
            keep.start()
    for d in order:
        lax.fori_loop(1, plane_size, lambda k, c: (plane_copy(d, k).wait_send(), c)[1], 0)
        if d:
            z_copy(d).wait()
    keep.wait()


def dispatch(tok_send, cot_send, select, plane_size, slots):
    z_count, rows, features = tok_send.shape
    out = jax.ShapeDtypeStruct((z_count, plane_size * slots, features), tok_send.dtype)
    vmem, any_space = pl.BlockSpec(memory_space=pltpu.VMEM), pl.BlockSpec(memory_space=pl.ANY)
    dma = pltpu.SemaphoreType.DMA
    return pl.pallas_call(
        functools.partial(dispatch_kernel, plane_size, slots),
        out_shape=(out, out),
        in_specs=[vmem] * 3,
        out_specs=(any_space, any_space),
        scratch_shapes=[
            pltpu.VMEM((2, z_count, rows, features), tok_send.dtype),
            pltpu.VMEM((2,) + out.shape, tok_send.dtype),
            dma((2, z_count)),
            dma((2, z_count)),
            dma((2, z_count, plane_size)),
            dma((2, z_count, plane_size)),
            dma((2, z_count)),
        ],
        compiler_params=pltpu.CompilerParams(
            collective_id=0, has_side_effects=True, vmem_limit_bytes=48 * 1024 * 1024
        ),
        name="dispatch",
    )(tok_send, cot_send, select)


def combine(back, comb, plane_size, slots):
    z_count, _, features = back.shape
    rows = comb.shape[1]
    vmem, any_space = pl.BlockSpec(memory_space=pltpu.VMEM), pl.BlockSpec(memory_space=pl.ANY)
    dma = pltpu.SemaphoreType.DMA
    return pl.pallas_call(
        functools.partial(combine_kernel, plane_size, slots),
        out_shape=jax.ShapeDtypeStruct((z_count, rows, features), back.dtype),
        in_specs=[any_space, vmem],
        out_specs=any_space,
        scratch_shapes=[
            pltpu.VMEM(back.shape, back.dtype),
            pltpu.VMEM((z_count, rows, features), back.dtype),
            dma((z_count,)),
            dma((z_count,)),
            dma((z_count, plane_size)),
            dma((z_count, plane_size)),
            dma((z_count,)),
            dma(()),
        ],
        compiler_params=pltpu.CompilerParams(
            collective_id=1, has_side_effects=True, vmem_limit_bytes=48 * 1024 * 1024
        ),
        name="combine",
    )(back, comb)


def local(tokens, routes, gates, w_gate, w_up, w_down, moe_out, norm_gain, out_grad):
    z_count, x_count, t_count = (lax.axis_size(name) for name in AXES)
    plane_size = x_count * t_count
    devices = z_count * plane_size
    z, x, t = (lax.axis_index(name) for name in AXES)
    own = x * t_count + t
    me = z * plane_size + own
    tok_rows, features = tokens.shape
    top_count = routes.shape[1]
    capacity = groups * tok_rows // devices
    slots = -(-capacity // 16) * 16
    group_rows = 3 * tok_rows // 8
    route_count = tok_rows * top_count
    bf16 = jnp.bfloat16

    saved_out = moe_out.astype(jnp.float32)
    scaled = norm_gain[None, :] * out_grad.astype(jnp.float32)
    stats = jnp.stack([jnp.sum(saved_out * saved_out, axis=1), jnp.sum(saved_out * scaled, axis=1)])
    packed = jnp.concatenate(
        [stats.reshape(-1), routes.T.reshape(-1).astype(jnp.float32), gates.T.reshape(-1)]
    )
    gathered = lax.all_gather(packed, AXES, axis=0, tiled=False)
    stat_count = stats.size
    ep_stats = lax.dynamic_slice(gathered, (me - t, 0), (t_count, stat_count))
    square_sum, cross_sum = jnp.sum(ep_stats.reshape(t_count, 2, -1), axis=0)
    all_ids = gathered[:, stat_count : stat_count + route_count].astype(jnp.int32)
    all_gates = gathered[:, stat_count + route_count :].astype(bf16).astype(jnp.float32)

    inv_rms = lax.rsqrt(square_sum / features + epsilon)
    expert_cot = (
        inv_rms[:, None] * scaled - saved_out * (inv_rms**3 * cross_sum / features)[:, None]
    ).astype(bf16)
    cot_rows = lax.all_to_all(expert_cot, "tp", split_axis=0, concat_axis=1, tiled=True)

    own_ids = routes.T.reshape(-1)
    own_group = routes[:, 0] // plane_size
    z_slot = own_group * group_rows + earlier_equal(own_group)
    pack = (jnp.arange(groups * group_rows, dtype=jnp.int32)[:, None] == z_slot[None, :]).astype(bf16)
    tok_send = jnp.dot(pack, tokens, preferred_element_type=jnp.float32).astype(bf16)
    cot_send = jnp.dot(pack, cot_rows, preferred_element_type=jnp.float32).astype(bf16)

    ids = lax.dynamic_index_in_dim(
        all_ids.reshape(z_count, plane_size, route_count), own, axis=1, keepdims=False
    )
    slot_of = (ids - z * plane_size) * slots + earlier_equal(ids)
    slot_of = jnp.where(ids // plane_size == z, slot_of, -1)
    group_of = ids[:, :tok_rows] // plane_size
    row_of = jnp.where(group_of == z, earlier_equal(group_of), -1)
    row_of = jnp.tile(row_of, (1, top_count))
    at_slot = (
        slot_of[:, None, :] == jnp.arange(plane_size * slots, dtype=jnp.int32)[None, :, None]
    ).astype(bf16)
    at_row = (row_of[:, None, :] == jnp.arange(group_rows, dtype=jnp.int32)[None, :, None]).astype(bf16)
    select = jnp.einsum("zsf,zrf->zsr", at_slot, at_row, preferred_element_type=jnp.float32).astype(bf16)
    spread = jnp.einsum("zrf,zsf->zrs", at_row, at_slot, preferred_element_type=jnp.float32).astype(bf16)

    hit = all_ids == me
    hit_rank = jnp.cumsum(hit.astype(jnp.int32), axis=1) - 1
    chosen = hit[:, None, :] & (
        hit_rank[:, None, :] == jnp.arange(slots, dtype=jnp.int32)[None, :, None]
    )
    weight = jnp.sum(jnp.where(chosen, all_gates[:, None, :], 0.0), axis=2).reshape(-1)[:, None]

    token_in, cot_in = dispatch(
        tok_send.reshape(groups, group_rows, features),
        cot_send.reshape(groups, group_rows, features),
        select,
        plane_size,
        slots,
    )
    row_block = token_in.reshape(devices * slots, features)
    cot_in = cot_in.reshape(devices * slots, features)
    w_gate_one = w_gate[0]
    w_up_one = w_up[0]
    w_down_one = w_down[0]
    pre_gate = jnp.dot(row_block, w_gate_one, preferred_element_type=jnp.float32)
    pre_up = jnp.dot(row_block, w_up_one, preferred_element_type=jnp.float32)
    sigmoid_gate = jax.nn.sigmoid(pre_gate)
    activated = pre_gate * sigmoid_gate
    hidden = activated * pre_up
    hid_grad = contract(cot_in, w_down_one, 1, 1)
    gate_grad = jnp.sum(hidden * hid_grad, axis=1).astype(bf16)
    d_hidden = weight * hid_grad
    d_gate = (d_hidden * pre_up * sigmoid_gate * (1.0 + pre_gate * (1.0 - sigmoid_gate))).astype(bf16)
    d_up = (d_hidden * activated).astype(bf16)
    token_back = (contract(d_gate, w_gate_one, 1, 1) + contract(d_up, w_up_one, 1, 1)).astype(bf16)
    scaled_cot = (weight * cot_in.astype(jnp.float32)).astype(bf16)
    grad_gate = contract(row_block, d_gate, 0, 0).astype(bf16)
    grad_up = contract(row_block, d_up, 0, 0).astype(bf16)
    grad_down = contract(hidden.astype(bf16), scaled_cot, 0, 0).astype(bf16)

    back_gates = lax.all_to_all(
        gate_grad.reshape(devices, slots), AXES, split_axis=0, concat_axis=0, tiled=True
    )
    back = combine(
        token_back.reshape(z_count, plane_size * slots, features), spread, plane_size, slots
    )
    token_grad = contract(pack, back.reshape(groups * group_rows, features), 0, 0).astype(bf16)
    own_slots = own_ids * slots + earlier_equal(own_ids)
    picked = own_slots[:, None] == jnp.arange(devices * slots, dtype=jnp.int32)[None, :]
    gates_grad = jnp.sum(
        jnp.where(picked, back_gates.reshape(1, -1).astype(jnp.float32), 0.0), axis=1
    ).astype(bf16)
    gates_grad = gates_grad.reshape(top_count, tok_rows).T
    return (token_grad, gates_grad, grad_gate[None], grad_up[None], grad_down[None])


def solution(mesh):
    ep, tp = mesh.shape["ep"], mesh.shape["tp"]
    cut = Mesh(mesh.devices.reshape(groups, ep // groups, tp), AXES)
    rows, ep_axes = P(AXES, None), ("z", "x")
    cube = P(AXES, None, None)
    return jax.shard_map(
        local,
        mesh=cut,
        in_specs=(rows, rows, rows, cube, cube, cube, P(ep_axes, "tp"), P("tp"), P(ep_axes, "tp")),
        out_specs=(rows, rows, cube, cube, cube),
        check_vma=False,
    )
```

```python
import functools

import jax
import jax.numpy as jnp
from jax import lax
from jax.experimental import pallas as pl
from jax.experimental.pallas import tpu as pltpu
from jax.sharding import Mesh
from jax.sharding import PartitionSpec as P

epsilon = 1e-06
groups = 4
MESH = pl.DeviceIdType.MESH
AXES = ("z", "x", "tp")


def contract(left, right, left_dim, right_dim):
    return lax.dot_general(
        left, right, (((left_dim,), (right_dim,)), ((), ())), preferred_element_type=jnp.float32
    )


def earlier_equal(ids):
    count = ids.shape[-1]
    place = jnp.arange(count, dtype=jnp.int32)
    same = (ids[..., :, None] == ids[..., None, :]) & (place[:, None] > place[None, :])
    return jnp.sum(same.astype(jnp.int32), axis=-1)


def places(plane_size):
    z, x, t = (lax.axis_index(name) for name in AXES)
    z_count, t_count = lax.axis_size("z"), lax.axis_size("tp")
    own = x * t_count + t

    def z_peer(d):
        return (lax.rem(z + d, z_count), x, t)

    def plane_peer(k):
        q = lax.rem(own + k, plane_size)
        return q, (z, q // t_count, lax.rem(q, t_count))

    return z, own, z_count, z_peer, plane_peer


def enter(z_count, plane_size, z_peer, plane_peer):
    barrier = pltpu.get_barrier_semaphore()
    for d in range(1, z_count):
        pl.semaphore_signal(barrier, inc=1, device_id=z_peer(d), device_id_type=MESH)

    def greet(k, carry):
        pl.semaphore_signal(barrier, inc=1, device_id=plane_peer(k)[1], device_id_type=MESH)
        return carry

    lax.fori_loop(1, plane_size, greet, 0)
    pl.semaphore_wait(barrier, z_count - 1 + plane_size - 1)


def columns_dot(left, read, write, features):
    chunk = min(512, features)

    def one(c, carry):
        cols = pl.ds(pl.multiple_of(c * chunk, chunk), chunk)
        write(cols, jnp.dot(left, read(cols), preferred_element_type=jnp.float32))
        return carry

    lax.fori_loop(0, features // chunk, one, 0)


def dispatch_kernel(
    plane_size, slots, tok_ref, cot_ref, sel_ref, tok_out, cot_out,
    zbuf, sbuf, zs_sem, zr_sem, ps_sem, pr_sem, loc_sem,
):
    z, own, z_count, z_peer, plane_peer = places(plane_size)
    features = tok_ref.shape[-1]
    sends, outs = (tok_ref, cot_ref), (tok_out, cot_out)
    enter(z_count, plane_size, z_peer, plane_peer)

    def z_copy(a, d):
        return pltpu.make_async_remote_copy(
            src_ref=sends[a].at[lax.rem(z + d, z_count)],
            dst_ref=zbuf.at[a, d],
            send_sem=zs_sem.at[a, d],
            recv_sem=zr_sem.at[a, d],
            device_id=z_peer(d),
            device_id_type=MESH,
        )

    def rows_of(q):
        return pl.ds(pl.multiple_of(q * slots, slots), slots)

    def plane_copy(a, d, k):
        q, device = plane_peer(k)
        src = lax.rem(z + z_count - d, z_count)
        return pltpu.make_async_remote_copy(
            src_ref=sbuf.at[a, d, rows_of(q)],
            dst_ref=outs[a].at[src, rows_of(own)],
            send_sem=ps_sem.at[a, d, k],
            recv_sem=pr_sem.at[a, d, k],
            device_id=device,
            device_id_type=MESH,
        )

    def own_copy(a, d):
        src = lax.rem(z + z_count - d, z_count)
        return pltpu.make_async_copy(
            sbuf.at[a, d, rows_of(own)], outs[a].at[src, rows_of(own)], loc_sem.at[a, d]
        )

    for a in range(2):
        for d in range(1, z_count):
            z_copy(a, d).start()
    for a, d in [(0, 0), (1, 0)] + [(a, d) for a in range(2) for d in range(1, z_count)]:
        src = lax.rem(z + z_count - d, z_count)
        if d:
            z_copy(a, d).wait_recv()

        def read(cols):
            return zbuf[a, d, :, cols] if d else sends[a][z, :, cols]

        def write(cols, value):
            sbuf[a, d, :, cols] = value.astype(sbuf.dtype)

        columns_dot(sel_ref[src], read, write, features)
        lax.fori_loop(1, plane_size, lambda k, c: (plane_copy(a, d, k).start(), c)[1], 0)
        own_copy(a, d).start()
    for a in range(2):
        for d in range(z_count):
            if d:
                z_copy(a, d).wait_send()
            own_copy(a, d).wait()
            lax.fori_loop(1, plane_size, lambda k, c: (plane_copy(a, d, k).wait(), c)[1], 0)


def combine_kernel(
    plane_size, slots, back_ref, gate_ref, comb_ref, out_ref, gate_out,
    rbuf, gbuf, cbuf, hbuf, zs_sem, zr_sem, ps_sem, pr_sem, loc_sem, own_sem,
):
    z, own, z_count, z_peer, plane_peer = places(plane_size)
    sources, landed, sums, outs = (gate_ref, back_ref), (gbuf, rbuf), (hbuf, cbuf), (gate_out, out_ref)
    enter(z_count, plane_size, z_peer, plane_peer)

    def rows_of(q):
        return pl.ds(pl.multiple_of(q * slots, slots), slots)

    def plane_copy(a, d, k):
        q, device = plane_peer(k)
        return pltpu.make_async_remote_copy(
            src_ref=sources[a].at[lax.rem(z + d, z_count), rows_of(q)],
            dst_ref=landed[a].at[d, rows_of(own)],
            send_sem=ps_sem.at[a, d, k],
            recv_sem=pr_sem.at[a, d, k],
            device_id=device,
            device_id_type=MESH,
        )

    def own_rows(a, d):
        return pltpu.make_async_copy(
            sources[a].at[lax.rem(z + d, z_count), rows_of(own)],
            landed[a].at[d, rows_of(own)],
            loc_sem.at[a, d],
        )

    def z_copy(a, d):
        return pltpu.make_async_remote_copy(
            src_ref=sums[a].at[d],
            dst_ref=outs[a].at[z],
            send_sem=zs_sem.at[a, d],
            recv_sem=zr_sem.at[a, d],
            device_id=z_peer(d),
            device_id_type=MESH,
        )

    keep = [pltpu.make_async_copy(sums[a].at[0], outs[a].at[z], own_sem.at[a]) for a in range(2)]
    order = list(range(1, z_count)) + [0]
    for d in order:
        for a in range(2):
            own_rows(a, d).start()
            lax.fori_loop(1, plane_size, lambda k, c: (plane_copy(a, d, k).start(), c)[1], 0)
    for d in order:
        for a in range(2):
            own_rows(a, d).wait()
            lax.fori_loop(1, plane_size, lambda k, c: (plane_copy(a, d, k).wait_recv(), c)[1], 0)

            def read(cols):
                return landed[a][d, :, cols]

            def write(cols, value):
                sums[a][d, :, cols] = value.astype(sums[a].dtype)

            columns_dot(comb_ref[lax.rem(z + d, z_count)], read, write, landed[a].shape[-1])
            if d:
                z_copy(a, d).start()
            else:
                keep[a].start()
    for d in order:
        for a in range(2):
            lax.fori_loop(1, plane_size, lambda k, c: (plane_copy(a, d, k).wait_send(), c)[1], 0)
            if d:
                z_copy(a, d).wait()
            else:
                keep[a].wait()


def share_kernel(devices, stat_ref, meta_ref, stat_out, meta_out, ss_sem, sr_sem, ms_sem, mr_sem):
    z, x, t = (lax.axis_index(name) for name in AXES)
    x_count, t_count = lax.axis_size("x"), lax.axis_size("tp")
    me = (z * x_count + x) * t_count + t

    def peer(k):
        q = lax.rem(me + k, devices)
        return (q // (x_count * t_count), lax.rem(q // t_count, x_count), lax.rem(q, t_count))

    def meta_copy(k):
        return pltpu.make_async_remote_copy(
            src_ref=meta_ref,
            dst_ref=meta_out.at[me],
            send_sem=ms_sem.at[k],
            recv_sem=mr_sem.at[k],
            device_id=peer(k),
            device_id_type=MESH,
        )

    def stat_copy(j):
        return pltpu.make_async_remote_copy(
            src_ref=stat_ref,
            dst_ref=stat_out.at[t],
            send_sem=ss_sem.at[j],
            recv_sem=sr_sem.at[j],
            device_id=(z, x, lax.rem(t + j, t_count)),
            device_id_type=MESH,
        )

    barrier = pltpu.get_barrier_semaphore()

    def greet(k, carry):
        pl.semaphore_signal(barrier, inc=1, device_id=peer(k), device_id_type=MESH)
        return carry

    lax.fori_loop(1, devices, greet, 0)
    pl.semaphore_wait(barrier, devices - 1)
    for j in range(1, t_count):
        stat_copy(j).start()
    lax.fori_loop(1, devices, lambda k, c: (meta_copy(k).start(), c)[1], 0)
    stat_out[t] = stat_ref[...]
    meta_out[me] = meta_ref[...]
    for j in range(1, t_count):
        stat_copy(j).wait()
    lax.fori_loop(1, devices, lambda k, c: (meta_copy(k).wait(), c)[1], 0)


def share(stats, meta, devices):
    vmem = pl.BlockSpec(memory_space=pltpu.VMEM)
    t_count = lax.axis_size("tp")
    dma = pltpu.SemaphoreType.DMA
    return pl.pallas_call(
        functools.partial(share_kernel, devices),
        out_shape=(
            jax.ShapeDtypeStruct((t_count,) + stats.shape, stats.dtype),
            jax.ShapeDtypeStruct((devices,) + meta.shape, meta.dtype),
        ),
        in_specs=[vmem] * 2,
        out_specs=(vmem, vmem),
        scratch_shapes=[dma((t_count,)), dma((t_count,)), dma((devices,)), dma((devices,))],
        compiler_params=pltpu.CompilerParams(collective_id=2, has_side_effects=True),
        name="share",
    )(stats, meta)


def dispatch(tok_send, cot_send, select, plane_size, slots):
    z_count, rows, features = tok_send.shape
    out = jax.ShapeDtypeStruct((z_count, plane_size * slots, features), tok_send.dtype)
    vmem, any_space = pl.BlockSpec(memory_space=pltpu.VMEM), pl.BlockSpec(memory_space=pl.ANY)
    dma = pltpu.SemaphoreType.DMA
    return pl.pallas_call(
        functools.partial(dispatch_kernel, plane_size, slots),
        out_shape=(out, out),
        in_specs=[vmem] * 3,
        out_specs=(any_space, any_space),
        scratch_shapes=[
            pltpu.VMEM((2, z_count, rows, features), tok_send.dtype),
            pltpu.VMEM((2,) + out.shape, tok_send.dtype),
            dma((2, z_count)),
            dma((2, z_count)),
            dma((2, z_count, plane_size)),
            dma((2, z_count, plane_size)),
            dma((2, z_count)),
        ],
        compiler_params=pltpu.CompilerParams(
            collective_id=0, has_side_effects=True, vmem_limit_bytes=48 * 1024 * 1024
        ),
        name="dispatch",
    )(tok_send, cot_send, select)


def combine(back, gate_back, comb, plane_size, slots):
    z_count, _, features = back.shape
    rows, lanes = comb.shape[1], gate_back.shape[-1]
    vmem, any_space = pl.BlockSpec(memory_space=pltpu.VMEM), pl.BlockSpec(memory_space=pl.ANY)
    dma = pltpu.SemaphoreType.DMA
    return pl.pallas_call(
        functools.partial(combine_kernel, plane_size, slots),
        out_shape=(
            jax.ShapeDtypeStruct((z_count, rows, features), back.dtype),
            jax.ShapeDtypeStruct((z_count, rows, lanes), back.dtype),
        ),
        in_specs=[any_space, any_space, vmem],
        out_specs=(any_space, any_space),
        scratch_shapes=[
            pltpu.VMEM(back.shape, back.dtype),
            pltpu.VMEM(gate_back.shape, back.dtype),
            pltpu.VMEM((z_count, rows, features), back.dtype),
            pltpu.VMEM((z_count, rows, lanes), back.dtype),
            dma((2, z_count)),
            dma((2, z_count)),
            dma((2, z_count, plane_size)),
            dma((2, z_count, plane_size)),
            dma((2, z_count)),
            dma((2,)),
        ],
        compiler_params=pltpu.CompilerParams(
            collective_id=1, has_side_effects=True, vmem_limit_bytes=48 * 1024 * 1024
        ),
        name="combine",
    )(back, gate_back, comb)


def local(tokens, routes, gates, w_gate, w_up, w_down, moe_out, norm_gain, out_grad):
    z_count, x_count, t_count = (lax.axis_size(name) for name in AXES)
    plane_size = x_count * t_count
    devices = z_count * plane_size
    z, x, t = (lax.axis_index(name) for name in AXES)
    own = x * t_count + t
    me = z * plane_size + own
    tok_rows, features = tokens.shape
    top_count = routes.shape[1]
    capacity = groups * tok_rows // devices
    slots = -(-capacity // 16) * 16
    group_rows = 3 * tok_rows // 8
    route_count = tok_rows * top_count
    bf16 = jnp.bfloat16
    lanes = 128

    saved_out = moe_out.astype(jnp.float32)
    scaled = norm_gain[None, :] * out_grad.astype(jnp.float32)
    stats = jnp.stack([jnp.sum(saved_out * saved_out, axis=1), jnp.sum(saved_out * scaled, axis=1)])
    meta = jnp.concatenate([routes.T.astype(jnp.float32), gates.T], axis=0).reshape(-1, lanes)
    all_stats, all_meta = share(stats.reshape(-1, lanes), meta, devices)
    square_sum, cross_sum = jnp.sum(all_stats.reshape(t_count, 2, -1), axis=0)
    all_meta = all_meta.reshape(devices, 2 * route_count)
    all_ids = all_meta[:, :route_count].astype(jnp.int32)
    all_gates = lax.reduce_precision(all_meta[:, route_count:], 8, 7)

    inv_rms = lax.rsqrt(square_sum / features + epsilon)
    expert_cot = (
        inv_rms[:, None] * scaled - saved_out * (inv_rms**3 * cross_sum / features)[:, None]
    ).astype(bf16)
    cot_rows = lax.all_to_all(expert_cot, "tp", split_axis=0, concat_axis=1, tiled=True)

    own_group = routes[:, 0] // plane_size
    z_slot = own_group * group_rows + earlier_equal(own_group)
    pack = (jnp.arange(groups * group_rows, dtype=jnp.int32)[:, None] == z_slot[None, :]).astype(bf16)
    tok_send = jnp.dot(pack, tokens, preferred_element_type=jnp.float32).astype(bf16)
    cot_send = jnp.dot(pack, cot_rows, preferred_element_type=jnp.float32).astype(bf16)

    ids = lax.dynamic_index_in_dim(
        all_ids.reshape(z_count, plane_size, route_count), own, axis=1, keepdims=False
    )
    slot_of = (ids - z * plane_size) * slots + earlier_equal(ids)
    slot_of = jnp.where(ids // plane_size == z, slot_of, -1)
    group_of = ids[:, :tok_rows] // plane_size
    row_of = jnp.where(group_of == z, earlier_equal(group_of), -1)
    row_of = jnp.tile(row_of, (1, top_count))
    at_slot = (
        slot_of[:, None, :] == jnp.arange(plane_size * slots, dtype=jnp.int32)[None, :, None]
    ).astype(bf16)
    at_row = (row_of[:, None, :] == jnp.arange(group_rows, dtype=jnp.int32)[None, :, None]).astype(bf16)
    select = jnp.einsum("zsf,zrf->zsr", at_slot, at_row, preferred_element_type=jnp.float32).astype(bf16)
    spread = jnp.einsum("zrf,zsf->zrs", at_row, at_slot, preferred_element_type=jnp.float32).astype(bf16)

    hit = all_ids == me
    hit_rank = jnp.cumsum(hit.astype(jnp.int32), axis=1) - 1
    chosen = hit[:, None, :] & (
        hit_rank[:, None, :] == jnp.arange(slots, dtype=jnp.int32)[None, :, None]
    )
    weight = jnp.sum(jnp.where(chosen, all_gates[:, None, :], 0.0), axis=2).reshape(-1)[:, None]
    column = jnp.arange(route_count, dtype=jnp.int32) // tok_rows
    which = jnp.sum(jnp.where(chosen, column[None, None, :], 0), axis=2).reshape(-1)

    token_in, cot_in = dispatch(
        tok_send.reshape(groups, group_rows, features),
        cot_send.reshape(groups, group_rows, features),
        select,
        plane_size,
        slots,
    )
    row_block = token_in.reshape(devices * slots, features)
    cot_in = cot_in.reshape(devices * slots, features)
    w_gate_one = w_gate[0]
    w_up_one = w_up[0]
    w_down_one = w_down[0]
    pre_gate = jnp.dot(row_block, w_gate_one, preferred_element_type=jnp.float32)
    pre_up = jnp.dot(row_block, w_up_one, preferred_element_type=jnp.float32)
    sigmoid_gate = jax.nn.sigmoid(pre_gate)
    activated = pre_gate * sigmoid_gate
    hidden = activated * pre_up
    hid_grad = contract(cot_in, w_down_one, 1, 1)
    gate_grad = jnp.sum(hidden * hid_grad, axis=1).astype(bf16)
    d_hidden = weight * hid_grad
    d_gate = (d_hidden * pre_up * sigmoid_gate * (1.0 + pre_gate * (1.0 - sigmoid_gate))).astype(bf16)
    d_up = (d_hidden * activated).astype(bf16)
    token_back = (contract(d_gate, w_gate_one, 1, 1) + contract(d_up, w_up_one, 1, 1)).astype(bf16)
    scaled_cot = (weight * cot_in.astype(jnp.float32)).astype(bf16)
    grad_gate = contract(row_block, d_gate, 0, 0).astype(bf16)
    grad_up = contract(row_block, d_up, 0, 0).astype(bf16)
    grad_down = contract(hidden.astype(bf16), scaled_cot, 0, 0).astype(bf16)

    gate_back = jnp.where(
        jnp.arange(lanes, dtype=jnp.int32)[None, :] == which[:, None], gate_grad[:, None], 0
    ).astype(bf16)
    back, gate_sums = combine(
        token_back.reshape(z_count, plane_size * slots, features),
        gate_back.reshape(z_count, plane_size * slots, lanes),
        spread,
        plane_size,
        slots,
    )
    token_grad = contract(pack, back.reshape(groups * group_rows, features), 0, 0).astype(bf16)
    gates_grad = contract(pack, gate_sums.reshape(groups * group_rows, lanes), 0, 0).astype(bf16)
    gates_grad = gates_grad[:, :top_count]
    return (token_grad, gates_grad, grad_gate[None], grad_up[None], grad_down[None])


def solution(mesh):
    ep, tp = mesh.shape["ep"], mesh.shape["tp"]
    cut = Mesh(mesh.devices.reshape(groups, ep // groups, tp), AXES)
    rows, ep_axes = P(AXES, None), ("z", "x")
    cube = P(AXES, None, None)
    return jax.shard_map(
        local,
        mesh=cut,
        in_specs=(rows, rows, rows, cube, cube, cube, P(ep_axes, "tp"), P("tp"), P(ep_axes, "tp")),
        out_specs=(rows, rows, cube, cube, cube),
        check_vma=False,
    )
```

```python
import functools

import jax
import jax.numpy as jnp
from jax import lax
from jax.experimental import pallas as pl
from jax.experimental.pallas import tpu as pltpu
from jax.sharding import Mesh
from jax.sharding import PartitionSpec as P

epsilon = 1e-06
groups = 4
MESH = pl.DeviceIdType.MESH
AXES = ("z", "x", "tp")


def contract(left, right, left_dim, right_dim):
    return lax.dot_general(
        left, right, (((left_dim,), (right_dim,)), ((), ())), preferred_element_type=jnp.float32
    )


def earlier_equal(ids):
    count = ids.shape[-1]
    place = jnp.arange(count, dtype=jnp.int32)
    same = (ids[..., :, None] == ids[..., None, :]) & (place[:, None] > place[None, :])
    return jnp.sum(same.astype(jnp.int32), axis=-1)


def places(plane_size):
    z, x, t = (lax.axis_index(name) for name in AXES)
    z_count, t_count = lax.axis_size("z"), lax.axis_size("tp")
    own = x * t_count + t

    def z_peer(d):
        return (lax.rem(z + d, z_count), x, t)

    def plane_peer(k):
        q = lax.rem(own + k, plane_size)
        return q, (z, q // t_count, lax.rem(q, t_count))

    return z, own, z_count, z_peer, plane_peer


def enter(z_count, plane_size, z_peer, plane_peer):
    barrier = pltpu.get_barrier_semaphore()
    for d in range(1, z_count):
        pl.semaphore_signal(barrier, inc=1, device_id=z_peer(d), device_id_type=MESH)

    def greet(k, carry):
        pl.semaphore_signal(barrier, inc=1, device_id=plane_peer(k)[1], device_id_type=MESH)
        return carry

    lax.fori_loop(1, plane_size, greet, 0)
    pl.semaphore_wait(barrier, z_count - 1 + plane_size - 1)


def columns_dot(left, read, write, features):
    chunk = min(512, features)

    def one(c, carry):
        cols = pl.ds(pl.multiple_of(c * chunk, chunk), chunk)
        write(cols, jnp.dot(left, read(cols), preferred_element_type=jnp.float32))
        return carry

    lax.fori_loop(0, features // chunk, one, 0)


def dispatch_kernel(
    plane_size, slots, tok_ref, sel_ref, pack_ref, moe_ref, grad_ref, gain_ref, coef_ref, tok_out, cot_out,
    cot_part, cot_rows, cot_send, zbuf, sbuf, ts_sem, tr_sem, zs_sem, zr_sem, ps_sem, pr_sem, loc_sem,
):
    z, own, z_count, z_peer, plane_peer = places(plane_size)
    x, t = lax.axis_index("x"), lax.axis_index("tp")
    t_count, part_rows, part_cols = cot_rows.shape
    group_rows, features = tok_ref.shape[1:]
    sends, outs = (tok_ref, cot_send), (tok_out, cot_out)
    enter(z_count, plane_size, z_peer, plane_peer)

    def z_copy(a, d):
        return pltpu.make_async_remote_copy(
            src_ref=sends[a].at[lax.rem(z + d, z_count)],
            dst_ref=zbuf.at[a, d],
            send_sem=zs_sem.at[a, d],
            recv_sem=zr_sem.at[a, d],
            device_id=z_peer(d),
            device_id_type=MESH,
        )

    def rows_of(q):
        return pl.ds(pl.multiple_of(q * slots, slots), slots)

    def plane_copy(a, d, k):
        q, device = plane_peer(k)
        src = lax.rem(z + z_count - d, z_count)
        return pltpu.make_async_remote_copy(
            src_ref=sbuf.at[a, d, rows_of(q)],
            dst_ref=outs[a].at[src, rows_of(own)],
            send_sem=ps_sem.at[a, d, k],
            recv_sem=pr_sem.at[a, d, k],
            device_id=device,
            device_id_type=MESH,
        )

    def own_copy(a, d):
        src = lax.rem(z + z_count - d, z_count)
        return pltpu.make_async_copy(
            sbuf.at[a, d, rows_of(own)], outs[a].at[src, rows_of(own)], loc_sem.at[a, d]
        )

    def part_copy(j):
        return pltpu.make_async_remote_copy(
            src_ref=cot_part.at[j],
            dst_ref=cot_rows.at[t],
            send_sem=ts_sem.at[j],
            recv_sem=tr_sem.at[j],
            device_id=(z, x, lax.rem(t + j, t_count)),
            device_id_type=MESH,
        )

    def spread_block(a, d):
        src = lax.rem(z + z_count - d, z_count)

        def read(cols):
            return zbuf[a, d, :, cols] if d else sends[a][z, :, cols]

        def write(cols, value):
            sbuf[a, d, :, cols] = value.astype(sbuf.dtype)

        columns_dot(sel_ref[src], read, write, features)
        lax.fori_loop(1, plane_size, lambda k, c: (plane_copy(a, d, k).start(), c)[1], 0)
        own_copy(a, d).start()

    for d in range(1, z_count):
        z_copy(0, d).start()
    block = 32
    for j in list(range(1, t_count)) + [0]:
        first = lax.rem(t + j, t_count) * part_rows

        def norm_rows(i, carry):
            rows = pl.ds(pl.multiple_of(first + i * block, block), block)
            scaled = gain_ref[...] * grad_ref[rows, :].astype(jnp.float32)
            saved_out = moe_ref[rows, :].astype(jnp.float32)
            value = coef_ref[rows, 0:1] * scaled - saved_out * coef_ref[rows, 1:2]
            here = pl.ds(pl.multiple_of(i * block, block), block)
            if j:
                cot_part[j, here, :] = value.astype(cot_part.dtype)
            else:
                cot_rows[t, here, :] = value.astype(cot_rows.dtype)
            return carry

        lax.fori_loop(0, part_rows // block, norm_rows, 0)
        if j:
            part_copy(j).start()
    spread_block(0, 0)
    for j in range(1, t_count):
        part_copy(j).wait_recv()
    for part in range(t_count):
        packed = jnp.dot(pack_ref[...], cot_rows[part], preferred_element_type=jnp.float32)
        packed = packed.astype(cot_send.dtype)
        for g in range(z_count):
            cot_send[g, :, part * part_cols : (part + 1) * part_cols] = packed[
                g * group_rows : (g + 1) * group_rows
            ]
    for d in range(1, z_count):
        z_copy(1, d).start()
    spread_block(1, 0)
    for a in range(2):
        for d in range(1, z_count):
            z_copy(a, d).wait_recv()
            spread_block(a, d)
    for j in range(1, t_count):
        part_copy(j).wait_send()
    for a in range(2):
        for d in range(z_count):
            if d:
                z_copy(a, d).wait_send()
            own_copy(a, d).wait()
            lax.fori_loop(1, plane_size, lambda k, c: (plane_copy(a, d, k).wait(), c)[1], 0)


def combine_kernel(
    plane_size, slots, back_ref, gate_ref, comb_ref, out_ref, gate_out,
    rbuf, gbuf, cbuf, hbuf, zs_sem, zr_sem, ps_sem, pr_sem, loc_sem, own_sem,
):
    z, own, z_count, z_peer, plane_peer = places(plane_size)
    sources, landed, sums, outs = (gate_ref, back_ref), (gbuf, rbuf), (hbuf, cbuf), (gate_out, out_ref)
    enter(z_count, plane_size, z_peer, plane_peer)

    def rows_of(q):
        return pl.ds(pl.multiple_of(q * slots, slots), slots)

    def plane_copy(a, d, k):
        q, device = plane_peer(k)
        return pltpu.make_async_remote_copy(
            src_ref=sources[a].at[lax.rem(z + d, z_count), rows_of(q)],
            dst_ref=landed[a].at[d, rows_of(own)],
            send_sem=ps_sem.at[a, d, k],
            recv_sem=pr_sem.at[a, d, k],
            device_id=device,
            device_id_type=MESH,
        )

    def own_rows(a, d):
        return pltpu.make_async_copy(
            sources[a].at[lax.rem(z + d, z_count), rows_of(own)],
            landed[a].at[d, rows_of(own)],
            loc_sem.at[a, d],
        )

    def z_copy(a, d):
        return pltpu.make_async_remote_copy(
            src_ref=sums[a].at[d],
            dst_ref=outs[a].at[z],
            send_sem=zs_sem.at[a, d],
            recv_sem=zr_sem.at[a, d],
            device_id=z_peer(d),
            device_id_type=MESH,
        )

    keep = [pltpu.make_async_copy(sums[a].at[0], outs[a].at[z], own_sem.at[a]) for a in range(2)]
    order = list(range(1, z_count)) + [0]
    for d in order:
        for a in range(2):
            own_rows(a, d).start()
            lax.fori_loop(1, plane_size, lambda k, c: (plane_copy(a, d, k).start(), c)[1], 0)
    for d in order:
        for a in range(2):
            own_rows(a, d).wait()
            lax.fori_loop(1, plane_size, lambda k, c: (plane_copy(a, d, k).wait_recv(), c)[1], 0)

            def read(cols):
                return landed[a][d, :, cols]

            def write(cols, value):
                sums[a][d, :, cols] = value.astype(sums[a].dtype)

            columns_dot(comb_ref[lax.rem(z + d, z_count)], read, write, landed[a].shape[-1])
            if d:
                z_copy(a, d).start()
            else:
                keep[a].start()
    for d in order:
        for a in range(2):
            lax.fori_loop(1, plane_size, lambda k, c: (plane_copy(a, d, k).wait_send(), c)[1], 0)
            if d:
                z_copy(a, d).wait()
            else:
                keep[a].wait()


def share_kernel(devices, stat_ref, meta_ref, stat_out, meta_out, ss_sem, sr_sem, ms_sem, mr_sem):
    z, x, t = (lax.axis_index(name) for name in AXES)
    x_count, t_count = lax.axis_size("x"), lax.axis_size("tp")
    me = (z * x_count + x) * t_count + t

    def peer(k):
        q = lax.rem(me + k, devices)
        return (q // (x_count * t_count), lax.rem(q // t_count, x_count), lax.rem(q, t_count))

    def meta_copy(k):
        return pltpu.make_async_remote_copy(
            src_ref=meta_ref,
            dst_ref=meta_out.at[me],
            send_sem=ms_sem.at[k],
            recv_sem=mr_sem.at[k],
            device_id=peer(k),
            device_id_type=MESH,
        )

    def stat_copy(j):
        return pltpu.make_async_remote_copy(
            src_ref=stat_ref,
            dst_ref=stat_out.at[t],
            send_sem=ss_sem.at[j],
            recv_sem=sr_sem.at[j],
            device_id=(z, x, lax.rem(t + j, t_count)),
            device_id_type=MESH,
        )

    barrier = pltpu.get_barrier_semaphore()

    def greet(k, carry):
        pl.semaphore_signal(barrier, inc=1, device_id=peer(k), device_id_type=MESH)
        return carry

    lax.fori_loop(1, devices, greet, 0)
    pl.semaphore_wait(barrier, devices - 1)
    for j in range(1, t_count):
        stat_copy(j).start()
    lax.fori_loop(1, devices, lambda k, c: (meta_copy(k).start(), c)[1], 0)
    stat_out[t] = stat_ref[...]
    meta_out[me] = meta_ref[...]
    for j in range(1, t_count):
        stat_copy(j).wait()
    lax.fori_loop(1, devices, lambda k, c: (meta_copy(k).wait(), c)[1], 0)


def share(stats, meta, devices):
    vmem = pl.BlockSpec(memory_space=pltpu.VMEM)
    t_count = lax.axis_size("tp")
    dma = pltpu.SemaphoreType.DMA
    return pl.pallas_call(
        functools.partial(share_kernel, devices),
        out_shape=(
            jax.ShapeDtypeStruct((t_count,) + stats.shape, stats.dtype),
            jax.ShapeDtypeStruct((devices,) + meta.shape, meta.dtype),
        ),
        in_specs=[vmem] * 2,
        out_specs=(vmem, vmem),
        scratch_shapes=[dma((t_count,)), dma((t_count,)), dma((devices,)), dma((devices,))],
        compiler_params=pltpu.CompilerParams(collective_id=2, has_side_effects=True),
        name="share",
    )(stats, meta)


def dispatch(tok_send, select, pack, moe_out, out_grad, gain, coefs, plane_size, slots):
    z_count, rows, features = tok_send.shape
    t_count = lax.axis_size("tp")
    part = (t_count, moe_out.shape[0] // t_count, moe_out.shape[1])
    out = jax.ShapeDtypeStruct((z_count, plane_size * slots, features), tok_send.dtype)
    vmem, any_space = pl.BlockSpec(memory_space=pltpu.VMEM), pl.BlockSpec(memory_space=pl.ANY)
    dma = pltpu.SemaphoreType.DMA
    return pl.pallas_call(
        functools.partial(dispatch_kernel, plane_size, slots),
        out_shape=(out, out),
        in_specs=[vmem] * 7,
        out_specs=(any_space, any_space),
        scratch_shapes=[
            pltpu.VMEM(part, tok_send.dtype),
            pltpu.VMEM(part, tok_send.dtype),
            pltpu.VMEM(tok_send.shape, tok_send.dtype),
            pltpu.VMEM((2, z_count, rows, features), tok_send.dtype),
            pltpu.VMEM((2,) + out.shape, tok_send.dtype),
            dma((t_count,)),
            dma((t_count,)),
            dma((2, z_count)),
            dma((2, z_count)),
            dma((2, z_count, plane_size)),
            dma((2, z_count, plane_size)),
            dma((2, z_count)),
        ],
        compiler_params=pltpu.CompilerParams(
            collective_id=0, has_side_effects=True, vmem_limit_bytes=48 * 1024 * 1024
        ),
        name="dispatch",
    )(tok_send, select, pack, moe_out, out_grad, gain, coefs)


def combine(back, gate_back, comb, plane_size, slots):
    z_count, _, features = back.shape
    rows, lanes = comb.shape[1], gate_back.shape[-1]
    vmem, any_space = pl.BlockSpec(memory_space=pltpu.VMEM), pl.BlockSpec(memory_space=pl.ANY)
    dma = pltpu.SemaphoreType.DMA
    return pl.pallas_call(
        functools.partial(combine_kernel, plane_size, slots),
        out_shape=(
            jax.ShapeDtypeStruct((z_count, rows, features), back.dtype),
            jax.ShapeDtypeStruct((z_count, rows, lanes), back.dtype),
        ),
        in_specs=[any_space, any_space, vmem],
        out_specs=(any_space, any_space),
        scratch_shapes=[
            pltpu.VMEM(back.shape, back.dtype),
            pltpu.VMEM(gate_back.shape, back.dtype),
            pltpu.VMEM((z_count, rows, features), back.dtype),
            pltpu.VMEM((z_count, rows, lanes), back.dtype),
            dma((2, z_count)),
            dma((2, z_count)),
            dma((2, z_count, plane_size)),
            dma((2, z_count, plane_size)),
            dma((2, z_count)),
            dma((2,)),
        ],
        compiler_params=pltpu.CompilerParams(
            collective_id=1, has_side_effects=True, vmem_limit_bytes=48 * 1024 * 1024
        ),
        name="combine",
    )(back, gate_back, comb)


def local(tokens, routes, gates, w_gate, w_up, w_down, moe_out, norm_gain, out_grad):
    z_count, x_count, t_count = (lax.axis_size(name) for name in AXES)
    plane_size = x_count * t_count
    devices = z_count * plane_size
    z, x, t = (lax.axis_index(name) for name in AXES)
    own = x * t_count + t
    me = z * plane_size + own
    tok_rows, features = tokens.shape
    top_count = routes.shape[1]
    capacity = groups * tok_rows // devices
    slots = -(-capacity // 16) * 16
    group_rows = 3 * tok_rows // 8
    route_count = tok_rows * top_count
    bf16 = jnp.bfloat16
    lanes = 128

    saved_out = moe_out.astype(jnp.float32)
    scaled = norm_gain[None, :] * out_grad.astype(jnp.float32)
    stats = jnp.stack([jnp.sum(saved_out * saved_out, axis=1), jnp.sum(saved_out * scaled, axis=1)])
    meta = jnp.concatenate([routes.T.astype(jnp.float32), gates.T], axis=0).reshape(-1, lanes)
    all_stats, all_meta = share(stats.reshape(-1, lanes), meta, devices)
    square_sum, cross_sum = jnp.sum(all_stats.reshape(t_count, 2, -1), axis=0)
    all_meta = all_meta.reshape(devices, 2 * route_count)
    all_ids = all_meta[:, :route_count].astype(jnp.int32)
    all_gates = lax.reduce_precision(all_meta[:, route_count:], 8, 7)

    inv_rms = lax.rsqrt(square_sum / features + epsilon)
    coefs = jnp.stack([inv_rms, inv_rms**3 * cross_sum / features], axis=1)

    own_group = routes[:, 0] // plane_size
    z_slot = own_group * group_rows + earlier_equal(own_group)
    pack = (jnp.arange(groups * group_rows, dtype=jnp.int32)[:, None] == z_slot[None, :]).astype(bf16)
    tok_send = jnp.dot(pack, tokens, preferred_element_type=jnp.float32).astype(bf16)

    ids = lax.dynamic_index_in_dim(
        all_ids.reshape(z_count, plane_size, route_count), own, axis=1, keepdims=False
    )
    slot_of = (ids - z * plane_size) * slots + earlier_equal(ids)
    slot_of = jnp.where(ids // plane_size == z, slot_of, -1)
    group_of = ids[:, :tok_rows] // plane_size
    row_of = jnp.where(group_of == z, earlier_equal(group_of), -1)
    row_of = jnp.tile(row_of, (1, top_count))
    at_slot = (
        slot_of[:, None, :] == jnp.arange(plane_size * slots, dtype=jnp.int32)[None, :, None]
    ).astype(bf16)
    at_row = (row_of[:, None, :] == jnp.arange(group_rows, dtype=jnp.int32)[None, :, None]).astype(bf16)
    select = jnp.einsum("zsf,zrf->zsr", at_slot, at_row, preferred_element_type=jnp.float32).astype(bf16)
    spread = jnp.einsum("zrf,zsf->zrs", at_row, at_slot, preferred_element_type=jnp.float32).astype(bf16)

    hit = all_ids == me
    hit_rank = jnp.cumsum(hit.astype(jnp.int32), axis=1) - 1
    chosen = hit[:, None, :] & (
        hit_rank[:, None, :] == jnp.arange(slots, dtype=jnp.int32)[None, :, None]
    )
    weight = jnp.sum(jnp.where(chosen, all_gates[:, None, :], 0.0), axis=2).reshape(-1)[:, None]
    column = jnp.arange(route_count, dtype=jnp.int32) // tok_rows
    which = jnp.sum(jnp.where(chosen, column[None, None, :], 0), axis=2).reshape(-1)

    token_in, cot_in = dispatch(
        tok_send.reshape(groups, group_rows, features),
        select,
        pack,
        moe_out,
        out_grad,
        norm_gain[None, :],
        coefs,
        plane_size,
        slots,
    )
    row_block = token_in.reshape(devices * slots, features)
    cot_in = cot_in.reshape(devices * slots, features)
    w_gate_one = w_gate[0]
    w_up_one = w_up[0]
    w_down_one = w_down[0]
    pre_gate = jnp.dot(row_block, w_gate_one, preferred_element_type=jnp.float32)
    pre_up = jnp.dot(row_block, w_up_one, preferred_element_type=jnp.float32)
    sigmoid_gate = jax.nn.sigmoid(pre_gate)
    activated = pre_gate * sigmoid_gate
    hidden = activated * pre_up
    hid_grad = contract(cot_in, w_down_one, 1, 1)
    gate_grad = jnp.sum(hidden * hid_grad, axis=1).astype(bf16)
    d_hidden = weight * hid_grad
    d_gate = (d_hidden * pre_up * sigmoid_gate * (1.0 + pre_gate * (1.0 - sigmoid_gate))).astype(bf16)
    d_up = (d_hidden * activated).astype(bf16)
    token_back = (contract(d_gate, w_gate_one, 1, 1) + contract(d_up, w_up_one, 1, 1)).astype(bf16)
    scaled_cot = (weight * cot_in.astype(jnp.float32)).astype(bf16)
    grad_gate = contract(row_block, d_gate, 0, 0).astype(bf16)
    grad_up = contract(row_block, d_up, 0, 0).astype(bf16)
    grad_down = contract(hidden.astype(bf16), scaled_cot, 0, 0).astype(bf16)

    gate_back = jnp.where(
        jnp.arange(lanes, dtype=jnp.int32)[None, :] == which[:, None], gate_grad[:, None], 0
    ).astype(bf16)
    back, gate_sums = combine(
        token_back.reshape(z_count, plane_size * slots, features),
        gate_back.reshape(z_count, plane_size * slots, lanes),
        spread,
        plane_size,
        slots,
    )
    token_grad = contract(pack, back.reshape(groups * group_rows, features), 0, 0).astype(bf16)
    gates_grad = contract(pack, gate_sums.reshape(groups * group_rows, lanes), 0, 0).astype(bf16)
    gates_grad = gates_grad[:, :top_count]
    return (token_grad, gates_grad, grad_gate[None], grad_up[None], grad_down[None])


def solution(mesh):
    ep, tp = mesh.shape["ep"], mesh.shape["tp"]
    cut = Mesh(mesh.devices.reshape(groups, ep // groups, tp), AXES)
    rows, ep_axes = P(AXES, None), ("z", "x")
    cube = P(AXES, None, None)
    return jax.shard_map(
        local,
        mesh=cut,
        in_specs=(rows, rows, rows, cube, cube, cube, P(ep_axes, "tp"), P("tp"), P(ep_axes, "tp")),
        out_specs=(rows, rows, cube, cube, cube),
        check_vma=False,
    )
```

```python
import functools

import jax
import jax.numpy as jnp
from jax import lax
from jax.experimental import pallas as pl
from jax.experimental.pallas import tpu as pltpu
from jax.sharding import Mesh
from jax.sharding import PartitionSpec as P

epsilon = 1e-06
groups = 4
MESH = pl.DeviceIdType.MESH
AXES = ("z", "x", "tp")


def contract(left, right, left_dim, right_dim):
    return lax.dot_general(
        left, right, (((left_dim,), (right_dim,)), ((), ())), preferred_element_type=jnp.float32
    )


def earlier_equal(ids):
    count = ids.shape[-1]
    place = jnp.arange(count, dtype=jnp.int32)
    same = (ids[..., :, None] == ids[..., None, :]) & (place[:, None] > place[None, :])
    return jnp.sum(same.astype(jnp.int32), axis=-1)


def places(plane_size):
    z, x, t = (lax.axis_index(name) for name in AXES)
    z_count, t_count = lax.axis_size("z"), lax.axis_size("tp")
    own = x * t_count + t

    def z_peer(d):
        return (lax.rem(z + d, z_count), x, t)

    def plane_peer(k):
        q = lax.rem(own + k, plane_size)
        return q, (z, q // t_count, lax.rem(q, t_count))

    return z, own, z_count, z_peer, plane_peer


def enter(z_count, plane_size, z_peer, plane_peer):
    barrier = pltpu.get_barrier_semaphore()
    for d in range(1, z_count):
        pl.semaphore_signal(barrier, inc=1, device_id=z_peer(d), device_id_type=MESH)

    def greet(k, carry):
        pl.semaphore_signal(barrier, inc=1, device_id=plane_peer(k)[1], device_id_type=MESH)
        return carry

    lax.fori_loop(1, plane_size, greet, 0)
    pl.semaphore_wait(barrier, z_count - 1 + plane_size - 1)


def columns_dot(left, read, write, features):
    chunk = min(512, features)

    def one(c, carry):
        cols = pl.ds(pl.multiple_of(c * chunk, chunk), chunk)
        write(cols, jnp.dot(left, read(cols), preferred_element_type=jnp.float32))
        return carry

    lax.fori_loop(0, features // chunk, one, 0)


def dispatch_kernel(
    plane_size, slots, tok_ref, sel_ref, pack_ref, moe_ref, grad_ref, gain_ref, coef_ref, tok_out, cot_out,
    cot_part, cot_rows, cot_send, zbuf, sbuf, ts_sem, tr_sem, zs_sem, zr_sem, ps_sem, pr_sem, loc_sem,
):
    z, own, z_count, z_peer, plane_peer = places(plane_size)
    x, t = lax.axis_index("x"), lax.axis_index("tp")
    t_count, part_rows, part_cols = cot_rows.shape
    group_rows, features = tok_ref.shape[1:]
    sends, outs = (tok_ref, cot_send), (tok_out, cot_out)
    enter(z_count, plane_size, z_peer, plane_peer)

    def z_copy(a, d):
        return pltpu.make_async_remote_copy(
            src_ref=sends[a].at[lax.rem(z + d, z_count)],
            dst_ref=zbuf.at[a, d],
            send_sem=zs_sem.at[a, d],
            recv_sem=zr_sem.at[a, d],
            device_id=z_peer(d),
            device_id_type=MESH,
        )

    def rows_of(q):
        return pl.ds(pl.multiple_of(q * slots, slots), slots)

    def plane_copy(a, d, k):
        q, device = plane_peer(k)
        src = lax.rem(z + z_count - d, z_count)
        return pltpu.make_async_remote_copy(
            src_ref=sbuf.at[a, d, rows_of(q)],
            dst_ref=outs[a].at[src, rows_of(own)],
            send_sem=ps_sem.at[a, d, k],
            recv_sem=pr_sem.at[a, d, k],
            device_id=device,
            device_id_type=MESH,
        )

    def own_copy(a, d):
        src = lax.rem(z + z_count - d, z_count)
        return pltpu.make_async_copy(
            sbuf.at[a, d, rows_of(own)], outs[a].at[src, rows_of(own)], loc_sem.at[a, d]
        )

    def part_copy(j):
        return pltpu.make_async_remote_copy(
            src_ref=cot_part.at[j],
            dst_ref=cot_rows.at[t],
            send_sem=ts_sem.at[j],
            recv_sem=tr_sem.at[j],
            device_id=(z, x, lax.rem(t + j, t_count)),
            device_id_type=MESH,
        )

    def spread_block(a, d):
        src = lax.rem(z + z_count - d, z_count)

        def read(cols):
            return zbuf[a, d, :, cols] if d else sends[a][z, :, cols]

        def write(cols, value):
            sbuf[a, d, :, cols] = value.astype(sbuf.dtype)

        columns_dot(sel_ref[src], read, write, features)
        lax.fori_loop(1, plane_size, lambda k, c: (plane_copy(a, d, k).start(), c)[1], 0)
        own_copy(a, d).start()

    for d in range(1, z_count):
        z_copy(0, d).start()
    spread_block(0, 0)
    block = 32
    for j in list(range(1, t_count)) + [0]:
        first = lax.rem(t + j, t_count) * part_rows

        def norm_rows(i, carry):
            rows = pl.ds(pl.multiple_of(first + i * block, block), block)
            scaled = gain_ref[...] * grad_ref[rows, :].astype(jnp.float32)
            saved_out = moe_ref[rows, :].astype(jnp.float32)
            value = coef_ref[rows, 0:1] * scaled - saved_out * coef_ref[rows, 1:2]
            here = pl.ds(pl.multiple_of(i * block, block), block)
            if j:
                cot_part[j, here, :] = value.astype(cot_part.dtype)
            else:
                cot_rows[t, here, :] = value.astype(cot_rows.dtype)
            return carry

        lax.fori_loop(0, part_rows // block, norm_rows, 0)
        if j:
            part_copy(j).start()
    z_copy(0, 1).wait_recv()
    spread_block(0, 1)
    for j in range(1, t_count):
        part_copy(j).wait_recv()
    for part in range(t_count):
        packed = jnp.dot(pack_ref[...], cot_rows[part], preferred_element_type=jnp.float32)
        packed = packed.astype(cot_send.dtype)
        for g in range(z_count):
            cot_send[g, :, part * part_cols : (part + 1) * part_cols] = packed[
                g * group_rows : (g + 1) * group_rows
            ]
    for d in range(1, z_count):
        z_copy(1, d).start()
    spread_block(1, 0)
    for a in range(2):
        for d in range(2 - a, z_count):
            z_copy(a, d).wait_recv()
            spread_block(a, d)
    for j in range(1, t_count):
        part_copy(j).wait_send()
    for a in range(2):
        for d in range(z_count):
            if d:
                z_copy(a, d).wait_send()
            own_copy(a, d).wait()
            lax.fori_loop(1, plane_size, lambda k, c: (plane_copy(a, d, k).wait(), c)[1], 0)


def combine_kernel(
    plane_size, slots, back_ref, gate_ref, comb_ref, out_ref, gate_out,
    rbuf, gbuf, cbuf, hbuf, zs_sem, zr_sem, ps_sem, pr_sem, loc_sem, own_sem,
):
    z, own, z_count, z_peer, plane_peer = places(plane_size)
    sources, landed, sums, outs = (gate_ref, back_ref), (gbuf, rbuf), (hbuf, cbuf), (gate_out, out_ref)
    enter(z_count, plane_size, z_peer, plane_peer)

    def rows_of(q):
        return pl.ds(pl.multiple_of(q * slots, slots), slots)

    def plane_copy(a, d, k):
        q, device = plane_peer(k)
        return pltpu.make_async_remote_copy(
            src_ref=sources[a].at[lax.rem(z + d, z_count), rows_of(q)],
            dst_ref=landed[a].at[d, rows_of(own)],
            send_sem=ps_sem.at[a, d, k],
            recv_sem=pr_sem.at[a, d, k],
            device_id=device,
            device_id_type=MESH,
        )

    def own_rows(a, d):
        return pltpu.make_async_copy(
            sources[a].at[lax.rem(z + d, z_count), rows_of(own)],
            landed[a].at[d, rows_of(own)],
            loc_sem.at[a, d],
        )

    def z_copy(a, d):
        return pltpu.make_async_remote_copy(
            src_ref=sums[a].at[d],
            dst_ref=outs[a].at[z],
            send_sem=zs_sem.at[a, d],
            recv_sem=zr_sem.at[a, d],
            device_id=z_peer(d),
            device_id_type=MESH,
        )

    keep = [pltpu.make_async_copy(sums[a].at[0], outs[a].at[z], own_sem.at[a]) for a in range(2)]
    order = list(range(1, z_count)) + [0]
    for d in order:
        for a in range(2):
            own_rows(a, d).start()
            lax.fori_loop(1, plane_size, lambda k, c: (plane_copy(a, d, k).start(), c)[1], 0)
    for d in order:
        for a in range(2):
            own_rows(a, d).wait()
            lax.fori_loop(1, plane_size, lambda k, c: (plane_copy(a, d, k).wait_recv(), c)[1], 0)

            def read(cols):
                return landed[a][d, :, cols]

            def write(cols, value):
                sums[a][d, :, cols] = value.astype(sums[a].dtype)

            columns_dot(comb_ref[lax.rem(z + d, z_count)], read, write, landed[a].shape[-1])
            if d:
                z_copy(a, d).start()
            else:
                keep[a].start()
    for d in order:
        for a in range(2):
            lax.fori_loop(1, plane_size, lambda k, c: (plane_copy(a, d, k).wait_send(), c)[1], 0)
            if d:
                z_copy(a, d).wait()
            else:
                keep[a].wait()


def share_kernel(devices, stat_ref, meta_ref, stat_out, meta_out, ss_sem, sr_sem, ms_sem, mr_sem):
    z, x, t = (lax.axis_index(name) for name in AXES)
    x_count, t_count = lax.axis_size("x"), lax.axis_size("tp")
    me = (z * x_count + x) * t_count + t

    def peer(k):
        q = lax.rem(me + k, devices)
        return (q // (x_count * t_count), lax.rem(q // t_count, x_count), lax.rem(q, t_count))

    def meta_copy(k):
        return pltpu.make_async_remote_copy(
            src_ref=meta_ref,
            dst_ref=meta_out.at[me],
            send_sem=ms_sem.at[k],
            recv_sem=mr_sem.at[k],
            device_id=peer(k),
            device_id_type=MESH,
        )

    def stat_copy(j):
        return pltpu.make_async_remote_copy(
            src_ref=stat_ref,
            dst_ref=stat_out.at[t],
            send_sem=ss_sem.at[j],
            recv_sem=sr_sem.at[j],
            device_id=(z, x, lax.rem(t + j, t_count)),
            device_id_type=MESH,
        )

    barrier = pltpu.get_barrier_semaphore()

    def greet(k, carry):
        pl.semaphore_signal(barrier, inc=1, device_id=peer(k), device_id_type=MESH)
        return carry

    lax.fori_loop(1, devices, greet, 0)
    pl.semaphore_wait(barrier, devices - 1)
    for j in range(1, t_count):
        stat_copy(j).start()
    lax.fori_loop(1, devices, lambda k, c: (meta_copy(k).start(), c)[1], 0)
    stat_out[t] = stat_ref[...]
    meta_out[me] = meta_ref[...]
    for j in range(1, t_count):
        stat_copy(j).wait()
    lax.fori_loop(1, devices, lambda k, c: (meta_copy(k).wait(), c)[1], 0)


def share(stats, meta, devices):
    vmem = pl.BlockSpec(memory_space=pltpu.VMEM)
    t_count = lax.axis_size("tp")
    dma = pltpu.SemaphoreType.DMA
    return pl.pallas_call(
        functools.partial(share_kernel, devices),
        out_shape=(
            jax.ShapeDtypeStruct((t_count,) + stats.shape, stats.dtype),
            jax.ShapeDtypeStruct((devices,) + meta.shape, meta.dtype),
        ),
        in_specs=[vmem] * 2,
        out_specs=(vmem, vmem),
        scratch_shapes=[dma((t_count,)), dma((t_count,)), dma((devices,)), dma((devices,))],
        compiler_params=pltpu.CompilerParams(
            collective_id=2, has_side_effects=True, vmem_limit_bytes=8 * 1024 * 1024
        ),
        name="share",
    )(stats, meta)


def grant(*arrays):
    total = 0
    for shape, item in arrays:
        size = item
        for extent in shape[:-1] + (max(shape[-1], 128),):
            size *= extent
        total += size
    return total + 6 * 1024 * 1024


def dispatch(tok_send, select, pack, moe_out, out_grad, gain, coefs, plane_size, slots):
    z_count, rows, features = tok_send.shape
    t_count = lax.axis_size("tp")
    part = (t_count, moe_out.shape[0] // t_count, moe_out.shape[1])
    out = jax.ShapeDtypeStruct((z_count, plane_size * slots, features), tok_send.dtype)
    vmem, any_space = pl.BlockSpec(memory_space=pltpu.VMEM), pl.BlockSpec(memory_space=pl.ANY)
    dma = pltpu.SemaphoreType.DMA
    limit = grant(
        (out.shape, 4), (tok_send.shape, 8), (part, 8), (select.shape, 2), (pack.shape, 2), (coefs.shape, 4)
    )
    return pl.pallas_call(
        functools.partial(dispatch_kernel, plane_size, slots),
        out_shape=(out, out),
        in_specs=[vmem] * 7,
        out_specs=(any_space, any_space),
        scratch_shapes=[
            pltpu.VMEM(part, tok_send.dtype),
            pltpu.VMEM(part, tok_send.dtype),
            pltpu.VMEM(tok_send.shape, tok_send.dtype),
            pltpu.VMEM((2, z_count, rows, features), tok_send.dtype),
            pltpu.VMEM((2,) + out.shape, tok_send.dtype),
            dma((t_count,)),
            dma((t_count,)),
            dma((2, z_count)),
            dma((2, z_count)),
            dma((2, z_count, plane_size)),
            dma((2, z_count, plane_size)),
            dma((2, z_count)),
        ],
        compiler_params=pltpu.CompilerParams(
            collective_id=0, has_side_effects=True, vmem_limit_bytes=limit
        ),
        name="dispatch",
    )(tok_send, select, pack, moe_out, out_grad, gain, coefs)


def combine(back, gate_back, comb, plane_size, slots):
    z_count, _, features = back.shape
    rows, lanes = comb.shape[1], gate_back.shape[-1]
    vmem, any_space = pl.BlockSpec(memory_space=pltpu.VMEM), pl.BlockSpec(memory_space=pl.ANY)
    dma = pltpu.SemaphoreType.DMA
    limit = grant((back.shape, 2), (gate_back.shape, 2), ((z_count, rows, features + lanes), 2), (comb.shape, 2))
    return pl.pallas_call(
        functools.partial(combine_kernel, plane_size, slots),
        out_shape=(
            jax.ShapeDtypeStruct((z_count, rows, features), back.dtype),
            jax.ShapeDtypeStruct((z_count, rows, lanes), back.dtype),
        ),
        in_specs=[any_space, any_space, vmem],
        out_specs=(any_space, any_space),
        scratch_shapes=[
            pltpu.VMEM(back.shape, back.dtype),
            pltpu.VMEM(gate_back.shape, back.dtype),
            pltpu.VMEM((z_count, rows, features), back.dtype),
            pltpu.VMEM((z_count, rows, lanes), back.dtype),
            dma((2, z_count)),
            dma((2, z_count)),
            dma((2, z_count, plane_size)),
            dma((2, z_count, plane_size)),
            dma((2, z_count)),
            dma((2,)),
        ],
        compiler_params=pltpu.CompilerParams(
            collective_id=1, has_side_effects=True, vmem_limit_bytes=limit
        ),
        name="combine",
    )(back, gate_back, comb)


def local(tokens, routes, gates, w_gate, w_up, w_down, moe_out, norm_gain, out_grad):
    z_count, x_count, t_count = (lax.axis_size(name) for name in AXES)
    plane_size = x_count * t_count
    devices = z_count * plane_size
    z, x, t = (lax.axis_index(name) for name in AXES)
    own = x * t_count + t
    me = z * plane_size + own
    tok_rows, features = tokens.shape
    top_count = routes.shape[1]
    capacity = groups * tok_rows // devices
    slots = -(-capacity // 16) * 16
    group_rows = 3 * tok_rows // 8
    route_count = tok_rows * top_count
    bf16 = jnp.bfloat16
    lanes = 128

    saved_out = moe_out.astype(jnp.float32)
    scaled = norm_gain[None, :] * out_grad.astype(jnp.float32)
    stats = jnp.stack([jnp.sum(saved_out * saved_out, axis=1), jnp.sum(saved_out * scaled, axis=1)])
    meta = jnp.concatenate([routes.T.astype(jnp.float32), gates.T], axis=0).reshape(-1, lanes)
    all_stats, all_meta = share(stats.reshape(-1, lanes), meta, devices)
    square_sum, cross_sum = jnp.sum(all_stats.reshape(t_count, 2, -1), axis=0)
    all_meta = all_meta.reshape(devices, 2 * route_count)
    all_ids = all_meta[:, :route_count].astype(jnp.int32)
    all_gates = lax.reduce_precision(all_meta[:, route_count:], 8, 7)

    inv_rms = lax.rsqrt(square_sum / features + epsilon)
    coefs = jnp.stack([inv_rms, inv_rms**3 * cross_sum / features], axis=1)

    own_group = routes[:, 0] // plane_size
    z_slot = own_group * group_rows + earlier_equal(own_group)
    pack = (jnp.arange(groups * group_rows, dtype=jnp.int32)[:, None] == z_slot[None, :]).astype(bf16)
    tok_send = jnp.dot(pack, tokens, preferred_element_type=jnp.float32).astype(bf16)

    ids = lax.dynamic_index_in_dim(
        all_ids.reshape(z_count, plane_size, route_count), own, axis=1, keepdims=False
    )
    slot_of = (ids - z * plane_size) * slots + earlier_equal(ids)
    slot_of = jnp.where(ids // plane_size == z, slot_of, -1)
    group_of = ids[:, :tok_rows] // plane_size
    row_of = jnp.where(group_of == z, earlier_equal(group_of), -1)
    row_of = jnp.tile(row_of, (1, top_count))
    at_slot = (
        slot_of[:, None, :] == jnp.arange(plane_size * slots, dtype=jnp.int32)[None, :, None]
    ).astype(bf16)
    at_row = (row_of[:, None, :] == jnp.arange(group_rows, dtype=jnp.int32)[None, :, None]).astype(bf16)
    select = jnp.einsum("zsf,zrf->zsr", at_slot, at_row, preferred_element_type=jnp.float32).astype(bf16)
    spread = jnp.einsum("zrf,zsf->zrs", at_row, at_slot, preferred_element_type=jnp.float32).astype(bf16)

    hit = all_ids == me
    hit_rank = jnp.cumsum(hit.astype(jnp.int32), axis=1) - 1
    chosen = hit[:, None, :] & (
        hit_rank[:, None, :] == jnp.arange(slots, dtype=jnp.int32)[None, :, None]
    )
    weight = jnp.sum(jnp.where(chosen, all_gates[:, None, :], 0.0), axis=2).reshape(-1)[:, None]
    column = jnp.arange(route_count, dtype=jnp.int32) // tok_rows
    which = jnp.sum(jnp.where(chosen, column[None, None, :], 0), axis=2).reshape(-1)

    token_in, cot_in = dispatch(
        tok_send.reshape(groups, group_rows, features),
        select,
        pack,
        moe_out,
        out_grad,
        norm_gain[None, :],
        coefs,
        plane_size,
        slots,
    )
    row_block = token_in.reshape(devices * slots, features)
    cot_in = cot_in.reshape(devices * slots, features)
    w_gate_one = w_gate[0]
    w_up_one = w_up[0]
    w_down_one = w_down[0]
    pre_gate = jnp.dot(row_block, w_gate_one, preferred_element_type=jnp.float32)
    pre_up = jnp.dot(row_block, w_up_one, preferred_element_type=jnp.float32)
    sigmoid_gate = jax.nn.sigmoid(pre_gate)
    activated = pre_gate * sigmoid_gate
    hidden = activated * pre_up
    hid_grad = contract(cot_in, w_down_one, 1, 1)
    gate_grad = jnp.sum(hidden * hid_grad, axis=1).astype(bf16)
    d_hidden = weight * hid_grad
    d_gate = (d_hidden * pre_up * sigmoid_gate * (1.0 + pre_gate * (1.0 - sigmoid_gate))).astype(bf16)
    d_up = (d_hidden * activated).astype(bf16)
    token_back = (contract(d_gate, w_gate_one, 1, 1) + contract(d_up, w_up_one, 1, 1)).astype(bf16)
    scaled_cot = (weight * cot_in.astype(jnp.float32)).astype(bf16)
    grad_gate = contract(row_block, d_gate, 0, 0).astype(bf16)
    grad_up = contract(row_block, d_up, 0, 0).astype(bf16)
    grad_down = contract(hidden.astype(bf16), scaled_cot, 0, 0).astype(bf16)

    gate_back = jnp.where(
        jnp.arange(lanes, dtype=jnp.int32)[None, :] == which[:, None], gate_grad[:, None], 0
    ).astype(bf16)
    back, gate_sums = combine(
        token_back.reshape(z_count, plane_size * slots, features),
        gate_back.reshape(z_count, plane_size * slots, lanes),
        spread,
        plane_size,
        slots,
    )
    token_grad = contract(pack, back.reshape(groups * group_rows, features), 0, 0).astype(bf16)
    gates_grad = contract(pack, gate_sums.reshape(groups * group_rows, lanes), 0, 0).astype(bf16)
    gates_grad = gates_grad[:, :top_count]
    return (token_grad, gates_grad, grad_gate[None], grad_up[None], grad_down[None])


def solution(mesh):
    ep, tp = mesh.shape["ep"], mesh.shape["tp"]
    cut = Mesh(mesh.devices.reshape(groups, ep // groups, tp), AXES)
    rows, ep_axes = P(AXES, None), ("z", "x")
    cube = P(AXES, None, None)
    return jax.shard_map(
        local,
        mesh=cut,
        in_specs=(rows, rows, rows, cube, cube, cube, P(ep_axes, "tp"), P("tp"), P(ep_axes, "tp")),
        out_specs=(rows, rows, cube, cube, cube),
        check_vma=False,
    )
```
